32 devices in a mesh: sp: 8 (over z, y), tp: 4 (over x, core).
Axes of the slice: x: 2, y: 2, z: 4, core: 2. Of those that a mesh axis runs over, the one named last changes fastest.
Arguments:
- conv_input: bfloat16 [2048, 2048], P('sp', 'tp'), may hold values from -6 to 6
- gate_branch: bfloat16 [2048, 2048], P('sp', 'tp'), may hold values from -6 to 6
- conv_taps: float32 [4, 2048], P(None, 'tp'), may hold values from -3 to 3
- narrow_maps: bfloat16 [2, 8, 128, 128], P(None, 'tp'), may hold values from -0.5 to 0.5
- wide_maps: bfloat16 [2, 4, 256, 256], P(None, 'tp'), may hold values from -0.375 to 0.375
- decay_param: float32 [2048], P('tp'), may hold values from 4.5 to 20
- decay_shift: float32 [2048, 2048], P('sp', 'tp'), may hold values from -0.75 to 0
- mixer_out: bfloat16 [2048, 2048], P('tp'), may hold values from -0.125 to 0.125
- stream: bfloat16 [2048, 2048], P(('sp', 'tp')), may hold values from -6 to 6
- norm_gain: float32 [2048], replicated, may hold values from 0.1 to 1.9
- routes: int32 [2048, 4], P('sp'), may hold values from 0 to 7, all different within a row; in each aligned block of 64 rows (0 to 63, 64 to 127, ...) at most 64 rows name the same one
- route_weights: float32 [2048, 4], P('sp'), may hold values from 0.05 to 0.5
- expert_gate: bfloat16 [8, 2048, 2048], P('sp', None, 'tp'), may hold values from -1 to 1
- expert_up: bfloat16 [8, 2048, 2048], P('sp', None, 'tp'), may hold values from -1 to 1
- expert_down: bfloat16 [8, 2048, 2048], P('sp', 'tp'), may hold values from -0.015625 to 0.015625
Outputs:
- layer_out: bfloat16 [2048, 2048], P(('sp', 'tp'))
The draws below stay inside these ranges and needn't reach their ends.
Inputs may be any that keep to these rules, and one draw needn't show every extreme that they name: `routes`: each row names 4 different experts. In each aligned block of 64 rows no expert is named more than 64 times, and in every draw some expert is named exactly 64 times in some block.
All inputs are finite; a program needn't handle non-finite values.
Results may differ from the reference program's by a relative error of at most 0.015.
Values may be sent and summed in bfloat16 or wider, within the bound.
A program may use at most 128 MiB of HBM per device.

```python
import math
import jax
import jax.numpy as jnp
import numpy as np
from jax import lax

D = 2048
HN = 128
HW = 256
WIDE_HEADS = 4
NARROW_HEADS = 8
RECURRENT_WIDTH = 2048
CONV = 4
FF = 2048
FF_PIECE = 512
TOP = 4
EXPERTS = 8
TOK_DEV = 256
TOK_LOCAL = 64
SEQUENCE_TOKENS = 2048
CAP = 64
N_TP = 4


def head_of_channel():
    channel = jnp.arange(RECURRENT_WIDTH, dtype=jnp.int32)
    segment = channel // (2 * HN + HW)
    within = channel % (2 * HN + HW)
    narrow_head = 2 * segment + within // HN
    return jnp.where(within < 2 * HN, narrow_head, 2 * WIDE_HEADS + segment)


def draw_decay_param(key, part):
    random_key_series = jax.random.split(jax.random.fold_in(key, 21), 3)
    fast_odds = 8
    fast_head = jax.random.randint(random_key_series[0], (3 * WIDE_HEADS,), 0, 16) < fast_odds
    fast_rate = jnp.exp(jax.random.uniform(random_key_series[1], (RECURRENT_WIDTH,), jnp.float32, math.log(1.0 / 50.0), math.log(1.0 / 30.0)))
    slow_rate = jnp.exp(jax.random.uniform(random_key_series[2], (RECURRENT_WIDTH,), jnp.float32, math.log(0.05), math.log(0.4))) / SEQUENCE_TOKENS
    step_rate = jnp.where(fast_head[head_of_channel()], fast_rate, slow_rate)
    return (-jnp.log(jnp.expm1(0.25 * step_rate))).astype(jnp.float32)


def draw_decay_shift(key, part):
    random_key_series = jax.random.split(jax.random.fold_in(key, 31), 3)
    block_count = SEQUENCE_TOKENS // TOK_DEV
    block_rate = jnp.exp(jax.random.uniform(random_key_series[0], (block_count, 1, RECURRENT_WIDTH), jnp.float32, math.log(0.1), math.log(1.0))) / SEQUENCE_TOKENS
    stable_level = -jnp.broadcast_to(block_rate, (block_count, TOK_DEV, RECURRENT_WIDTH)).reshape(SEQUENCE_TOKENS, RECURRENT_WIDTH)
    spike_position = jax.random.randint(random_key_series[1], (2,), 0, SEQUENCE_TOKENS)
    spike_hit = jnp.any(jnp.arange(SEQUENCE_TOKENS)[:, None] == spike_position[None, :], axis=1).astype(jnp.float32)
    spike_magnitude = jax.random.uniform(random_key_series[2], (1, RECURRENT_WIDTH), jnp.float32, math.log(0.5), math.log(0.8))
    return (stable_level + spike_hit[:, None] * spike_magnitude).astype(jnp.float32)


def expert_matrix(key, salt_value):
    key_pair = jax.random.split(jax.random.fold_in(key, salt_value), 2)
    column_scale = jnp.exp(jax.random.uniform(key_pair[0], (EXPERTS, FF), jnp.float32, math.log(0.5), math.log(12.0)))

    def one_expert(inputs):
        expert_index, scale_row = inputs
        expert_key = jax.random.fold_in(key_pair[1], expert_index)
        entries = jax.random.normal(expert_key, (D, FF), jnp.float32)
        return jnp.clip(entries * scale_row[None, :] * D ** (-0.5), -1.0, 1.0).astype(jnp.bfloat16)
    return lax.map(one_expert, (jnp.arange(EXPERTS), column_scale))


def draw_expert_gate(key, part):
    return expert_matrix(key, 41)


def draw_expert_up(key, part):
    return expert_matrix(key, 42)


def shard_levels(key, dims, cuts, least, high):
    loudness, own = 1.0, jax.random.fold_in(key, 6)
    for dim, blocks in cuts:
        heights = jnp.exp(jax.random.uniform(jax.random.fold_in(own, dim), (blocks,), jnp.float32, least / len(cuts), high / len(cuts)))
        loudness = loudness * jnp.repeat(heights, dims[dim] // blocks).reshape([-1 if axis == dim else 1 for axis in range(len(dims))])
    return loudness


def assign_block(key, own, number, rows, amount, top, limit, lean):
    sequence = jax.random.permutation(key, amount)
    packed, common = load_shares(amount, rows * top, limit, lean, True), load_shares(amount, rows * top, limit, lean, False)
    places = jnp.arange(amount)

    def named(sizes, turn):
        used = int((sizes > 0).sum())
        fixed = max(1, used // 4)
        moved = fixed + (places - fixed + turn * (used - fixed)) % max(1, amount - fixed)
        return jnp.zeros((amount,), jnp.int32).at[sequence[jnp.where(places < fixed, places, moved)]].set(jnp.asarray(sizes, jnp.int32))

    sizes = jnp.where(number % 4 == 0, named(packed, number // 4), named(common, number - number // 4 - 1))
    mixed = jax.random.permutation(jax.random.fold_in(own, 3), amount)
    source_of, sink = mixed[0:amount // 2 * 2:2], mixed[1:amount // 2 * 2:2]
    margin = jnp.minimum(sizes[source_of] - 1, limit - sizes[sink]) // 2
    margin = jnp.where((source_of == sequence[0]) | (sink == sequence[0]) | (sizes[sink] == 0), 0, jnp.maximum(margin, 0))
    moved = jax.random.randint(jax.random.fold_in(own, 4), (amount // 2,), 0, 1 << 20) % (margin + 1)
    sizes = sizes.at[source_of].add(-moved).at[sink].add(moved)
    labels = jnp.searchsorted(jnp.cumsum(sizes), jnp.arange(rows * top), side="right").astype(jnp.int32)
    grid = labels.reshape(top, rows).T
    grid = grid[jax.random.permutation(jax.random.fold_in(own, 1), rows)]
    turn = jax.random.randint(jax.random.fold_in(own, 2), (rows, 1), 0, top)
    return jnp.take_along_axis(grid, (jnp.arange(top)[None, :] + turn) % top, axis=1)


def load_shares(amount, total, most, lean, full):
    weights = [(1 << 20) // math.isqrt(rank ** lean) + 1 for rank in range(1, amount + 1)]
    largest = most if full else min(most, max(-(-total // amount), total * weights[0] // sum(weights)))
    least = 1 if total - largest >= amount - 1 else 0
    holding, rest = [largest] + [least] * (amount - 1), total - largest - least * (amount - 1)
    while rest > 0:
        movable = [i for i in range(1, amount) if holding[i] < largest] or [i for i in range(1, amount) if holding[i] < most]
        whole, budget = sum([weights[i] for i in movable]), rest
        for i in movable:
            extra = min(most - holding[i], max(1, budget * weights[i] // whole), rest)
            holding[i] = holding[i] + extra
            rest = rest - extra
    return np.array(holding)


def bell_draw(stream_key, shape, spread, reach, cuts=(), kind=jnp.bfloat16):
    drawn = spread * jax.random.normal(stream_key, shape, jnp.float32)
    if cuts:
        drawn = drawn * shard_levels(stream_key, shape, cuts, -0.22, 0.18)
    return jnp.clip(drawn, -reach, reach).astype(kind)


def setup_inputs(seed: int = 0) -> dict:
    key_list = jax.random.split(jax.random.key(seed), 16)
    conv_input = bell_draw(key_list[0], (SEQUENCE_TOKENS, RECURRENT_WIDTH), 1.0, 6.0, ((0, 8), (1, 4)))
    gate_branch = bell_draw(key_list[1], (SEQUENCE_TOKENS, RECURRENT_WIDTH), 1.0, 6.0, ((0, 8), (1, 4)))
    conv_taps = bell_draw(key_list[2], (CONV, RECURRENT_WIDTH), 0.5, 3.0, ((1, 4),), jnp.float32)
    narrow_maps = bell_draw(key_list[3], (2, NARROW_HEADS, HN, HN), HN ** -0.5, 0.5, ((1, 4),))
    wide_maps = bell_draw(key_list[4], (2, WIDE_HEADS, HW, HW), HW ** -0.5, 0.375, ((1, 4),))
    decay_param = draw_decay_param(jax.random.fold_in(key_list[15], 71), 0)
    decay_shift = draw_decay_shift(jax.random.fold_in(key_list[15], 71), 0)
    mixer_out = bell_draw(key_list[7], (RECURRENT_WIDTH, D), RECURRENT_WIDTH ** -0.5, 0.125, ((0, 4),))
    stream = bell_draw(key_list[8], (SEQUENCE_TOKENS, D), 1.0, 6.0, ((0, 32),))
    norm_gain = jnp.clip(1.0 + 0.18 * jax.random.normal(key_list[9], (D,), jnp.float32), 0.1, 1.9)
    routes_keys = jax.random.split(jax.random.fold_in(key_list[10], 1), SEQUENCE_TOKENS // TOK_LOCAL)
    routes_turns = jax.random.permutation(jax.random.fold_in(key_list[10], 3), SEQUENCE_TOKENS // TOK_LOCAL)
    routes = jax.vmap(lambda own, number: assign_block(jax.random.fold_in(key_list[10], 2), own, number, TOK_LOCAL, EXPERTS, TOP, CAP, 2))(routes_keys, routes_turns).reshape((SEQUENCE_TOKENS, TOP))
    route_weights = jnp.clip(0.05 + 0.45 * jax.random.uniform(key_list[11], (SEQUENCE_TOKENS, TOP), jnp.float32) ** shard_levels(key_list[11], (SEQUENCE_TOKENS, TOP), ((0, 8),), -0.2, 0.2), 0.05, 0.5)
    expert_gate = draw_expert_gate(jax.random.fold_in(key_list[15], 71), 0)
    expert_up = draw_expert_up(jax.random.fold_in(key_list[15], 71), 0)
    expert_down = bell_draw(key_list[14], (EXPERTS, FF, D), (FF * 64) ** -0.5, 0.015625, ((0, 8), (1, 4)))
    return dict(conv_input=conv_input, gate_branch=gate_branch, conv_taps=conv_taps, narrow_maps=narrow_maps, wide_maps=wide_maps, decay_param=decay_param, decay_shift=decay_shift, mixer_out=mixer_out, stream=stream, norm_gain=norm_gain, routes=routes, route_weights=route_weights, expert_gate=expert_gate, expert_up=expert_up, expert_down=expert_down)


NORM_EPSILON = 1e-06
CLAMP_LIMIT = 7.0
GATE_SLOPE = 1.702
DECAY_SCALE = 8.0

def combine_steps(earlier, later):
    return (earlier[0] * later[0], later[0] * earlier[1] + later[1])

def head_maps(convolved, narrow_maps, wide_maps):
    seq_rows = convolved.shape[0]
    segments = convolved.reshape(seq_rows, WIDE_HEADS, 2 * HN + HW).astype(jnp.float32)
    narrow = segments[:, :, :2 * HN].reshape(seq_rows, 2 * WIDE_HEADS, HN)
    wide_part = segments[:, :, 2 * HN:]
    narrow_pre = jnp.einsum('rhi,mhio->mrho', narrow, narrow_maps.astype(jnp.float32))
    wide_pre = jnp.einsum('rhi,mhio->mrho', wide_part, wide_maps.astype(jnp.float32))
    narrow_pre = narrow_pre.reshape(2, seq_rows, WIDE_HEADS, 2 * HN)
    return jnp.concatenate([narrow_pre, wide_pre], axis=3).reshape(2, seq_rows, RECURRENT_WIDTH)

def clamp_units(gate_pre, up_pre):
    clamped = jnp.minimum(gate_pre, CLAMP_LIMIT)
    upper = jnp.clip(up_pre, -CLAMP_LIMIT, CLAMP_LIMIT)
    return (upper + 1.0) * clamped * jax.nn.sigmoid(GATE_SLOPE * clamped)

def reference(conv_input, gate_branch, conv_taps, narrow_maps, wide_maps, decay_param, decay_shift, mixer_out, stream, norm_gain, routes, route_weights, expert_gate, expert_up, expert_down):
    padded = jnp.pad(conv_input.astype(jnp.float32), ((CONV - 1, 0), (0, 0)))
    convolved = jnp.zeros((SEQUENCE_TOKENS, RECURRENT_WIDTH), jnp.float32)
    for offset in range(CONV):
        convolved = convolved + padded[offset:offset + SEQUENCE_TOKENS] * conv_taps[offset]
    convolved = convolved.astype(jnp.bfloat16)
    gate_pre = head_maps(convolved, narrow_maps, wide_maps)
    log_decay = -DECAY_SCALE * jax.nn.sigmoid(gate_pre[0]) * jax.nn.softplus(-decay_param) + decay_shift
    driving = jnp.sqrt(-jnp.expm1(2.0 * log_decay)) * jax.nn.sigmoid(gate_pre[1]) * convolved.astype(jnp.float32)
    _, recurrent = lax.associative_scan(combine_steps, (jnp.exp(log_decay), driving), axis=0)
    gated_rows = (recurrent * jax.nn.gelu(gate_branch.astype(jnp.float32))).astype(jnp.bfloat16)
    mixer_sum = jnp.dot(gated_rows, mixer_out, preferred_element_type=jnp.float32)
    hidden = (stream.astype(jnp.float32) + mixer_sum).astype(jnp.bfloat16)
    hidden_f = hidden.astype(jnp.float32)
    normed = (hidden_f * lax.rsqrt(lax.optimization_barrier(jnp.mean(hidden_f * hidden_f, axis=-1, keepdims=True)) + NORM_EPSILON) * norm_gain).astype(jnp.bfloat16)
    blocks = SEQUENCE_TOKENS // TOK_LOCAL
    flat_routes = routes.reshape(blocks, TOK_LOCAL * TOP)
    onehot = (flat_routes[:, :, None] == jnp.arange(EXPERTS, dtype=jnp.int32)[None, None, :]).astype(jnp.int32)
    slot_rank = lax.optimization_barrier(jnp.sum(jnp.cumsum(onehot, axis=1) * onehot, axis=2)) - 1
    block_index = jnp.arange(blocks, dtype=jnp.int32)[:, None]
    slot_index = flat_routes * (blocks * CAP) + block_index * CAP + slot_rank
    token_index = block_index * TOK_LOCAL + jnp.arange(TOK_LOCAL * TOP, dtype=jnp.int32)[None, :] // TOP
    slot_token = jnp.zeros((EXPERTS * blocks * CAP,), jnp.int32).at[slot_index.reshape(-1)].set(token_index.reshape(-1).astype(jnp.int32))
    slot_weight = jnp.zeros((EXPERTS * blocks * CAP,), route_weights.dtype).at[slot_index.reshape(-1)].set(route_weights.reshape(-1))
    slot_token = slot_token.reshape(EXPERTS, blocks * CAP)
    slot_weight = slot_weight.reshape(EXPERTS, blocks * CAP)

    def one_expert(combined, inputs):
        tokens_here, weights_here, gate_here, up_here, down_here = inputs
        picked = normed[tokens_here]
        gate_val = jnp.dot(picked, gate_here, preferred_element_type=jnp.float32)
        up_val = jnp.dot(picked, up_here, preferred_element_type=jnp.float32)
        activation = clamp_units(gate_val, up_val).astype(jnp.bfloat16)
        summed = jnp.zeros((picked.shape[0], D), jnp.float32)
        for piece_index in range(N_TP):
            first = piece_index * FF_PIECE
            partial_value = jnp.dot(activation[:, first:first + FF_PIECE], down_here[first:first + FF_PIECE], preferred_element_type=jnp.float32).astype(jnp.bfloat16)
            partial_value = lax.optimization_barrier(partial_value)
            summed = summed + partial_value.astype(jnp.float32)
        expert_out = lax.optimization_barrier(summed.astype(jnp.bfloat16)).astype(jnp.float32)
        combined = combined.at[tokens_here].add(weights_here[:, None] * expert_out)
        return (combined, None)
    combined, _ = lax.scan(one_expert, jnp.zeros((SEQUENCE_TOKENS, D), jnp.float32), (slot_token, slot_weight, expert_gate, expert_up, expert_down))
    return (hidden_f + combined).astype(jnp.bfloat16)
```

```python
import functools

import jax
import jax.numpy as jnp
from jax import lax
from jax.experimental import pallas as pl
from jax.experimental.pallas import tpu as pltpu
from jax.sharding import PartitionSpec as P

NORM_EPSILON = 1e-06
CLAMP_LIMIT = 7.0
GATE_SLOPE = 1.702
DECAY_SCALE = 8.0


def shifted(block, axis, distance):
    devices = range(lax.axis_size(axis))
    route = [(i - distance, i) for i in devices if i - distance in devices]
    return lax.ppermute(block, axis, route)


def clamp_units(gate_pre, up_pre):
    clamped = jnp.minimum(gate_pre, CLAMP_LIMIT)
    upper = jnp.clip(up_pre, -CLAMP_LIMIT, CLAMP_LIMIT)
    return (upper + 1.0) * clamped * jax.nn.sigmoid(GATE_SLOPE * clamped)


def slot_ranks(flat_routes, expert_total):
    onehot = (
        flat_routes[:, :, None] == jnp.arange(expert_total, dtype=jnp.int32)[None, None, :]
    ).astype(jnp.int32)
    return jnp.sum(jnp.cumsum(onehot, axis=1) * onehot, axis=2) - 1


def take_rows(source_rows, slot_source):
    filled = slot_source >= 0
    picked = source_rows[jnp.maximum(slot_source, 0)]
    return jnp.where(filled[:, None], picked, jnp.zeros_like(picked))


def expert_work(arrived, expert_gate, expert_up, expert_down):
    local_experts = expert_gate.shape[0]
    buffer_shape = arrived.shape
    grouped = arrived.reshape(
        buffer_shape[0] // local_experts,
        local_experts,
        buffer_shape[1] * buffer_shape[2],
        buffer_shape[3],
    )
    gate_pre = jnp.einsum(
        "sxcd,xdf->sxcf", grouped, expert_gate, preferred_element_type=jnp.float32
    )
    up_pre = jnp.einsum("sxcd,xdf->sxcf", grouped, expert_up, preferred_element_type=jnp.float32)
    activation = clamp_units(gate_pre, up_pre).astype(jnp.bfloat16)
    partial_value = jnp.einsum(
        "sxcf,xfd->sxcd", activation, expert_down, preferred_element_type=jnp.float32
    )
    return partial_value.reshape(buffer_shape)


LANES = 128
SUBLANES = 8
DX, DY, DC = 1, 2, 4
SERIES_LIMIT = 0.05


def mix_kernel(
    head_ref, conv_ref, taps_ref, narrow_ref, wide_ref, soft_ref, shift_ref,
    factor_ref, state_ref, padded, log_keep, drive_keep,
):
    rows, channels = conv_ref.shape
    taps = taps_ref.shape[0]
    padded[0:SUBLANES, :] = head_ref[...]
    padded[SUBLANES:, :] = conv_ref[...].astype(jnp.float32)
    total = jnp.zeros((rows, channels), jnp.float32)
    for k in range(taps):
        total = total + padded[pl.ds(SUBLANES - taps + 1 + k, rows), :] * taps_ref[k : k + 1, :]
    convolved = total.astype(jnp.bfloat16)
    narrow_size, wide_size = narrow_ref.shape[2], wide_ref.shape[2]
    spans = []
    for j in range(wide_ref.shape[1]):
        base = j * (2 * narrow_size + wide_size)
        spans.append((base, narrow_size, narrow_ref, 2 * j))
        spans.append((base + narrow_size, narrow_size, narrow_ref, 2 * j + 1))
        spans.append((base + 2 * narrow_size, wide_size, wide_ref, j))
    for start, size, maps, head in spans:
        piece = convolved[:, start : start + size]
        decay_pre = jnp.dot(piece, maps[0, head], preferred_element_type=jnp.float32)
        input_pre = jnp.dot(piece, maps[1, head], preferred_element_type=jnp.float32)
        cols = slice(start, start + size)
        log_decay = (
            -DECAY_SCALE * jax.nn.sigmoid(decay_pre) * soft_ref[:, cols] + shift_ref[:, cols]
        )
        decay = jnp.exp(log_decay)
        y = 2.0 * log_decay
        series = -y * (1.0 + y * (0.5 + y * (1.0 / 6.0 + y * (1.0 / 24.0 + y * (1.0 / 120.0)))))
        lost = jnp.where(y > -SERIES_LIMIT, series, 1.0 - decay * decay)
        log_keep[:, cols] = decay
        drive_keep[:, cols] = (
            jnp.sqrt(lost) * jax.nn.sigmoid(input_pre) * piece.astype(jnp.float32)
        )
    row_id = lax.broadcasted_iota(jnp.int32, (SUBLANES, channels), 0)

    def tile(i, carry):
        product, state = carry
        at = pl.ds(pl.multiple_of(i * SUBLANES, SUBLANES), SUBLANES)
        a, b = log_keep[at, :], drive_keep[at, :]
        step = 1
        while step < SUBLANES:
            inside = row_id >= step
            a_before = jnp.where(inside, pltpu.roll(a, step, 0), 1.0)
            b_before = jnp.where(inside, pltpu.roll(b, step, 0), 0.0)
            b = a * b_before + b
            a = a * a_before
            step *= 2
        b = b + a * state
        a = a * product
        factor_ref[at, :] = a
        state_ref[at, :] = b
        last = slice(SUBLANES - 1, SUBLANES)
        return (a[last, :], b[last, :])

    lax.fori_loop(
        0,
        rows // SUBLANES,
        tile,
        (jnp.ones((1, channels), jnp.float32), jnp.zeros((1, channels), jnp.float32)),
    )


def mix_local(head, conv_input, conv_taps, narrow_maps, wide_maps, soft, decay_shift):
    shape = conv_input.shape
    flat = jax.ShapeDtypeStruct(shape, jnp.float32)
    return pl.pallas_call(
        mix_kernel,
        out_shape=(flat, flat),
        in_specs=[pl.BlockSpec(memory_space=pltpu.VMEM)] * 7,
        out_specs=(pl.BlockSpec(memory_space=pltpu.VMEM),) * 2,
        scratch_shapes=[
            pltpu.VMEM((shape[0] + SUBLANES, shape[1]), jnp.float32),
            pltpu.VMEM(shape, jnp.float32),
            pltpu.VMEM(shape, jnp.float32),
        ],
        compiler_params=pltpu.CompilerParams(vmem_limit_bytes=32 * 1024 * 1024),
    )(head, conv_input, conv_taps, narrow_maps, wide_maps, soft, decay_shift)


def moe_kernel(
    depth, ext_ref, hid_ref, gate_hbm, up_hbm, down_hbm, out_ref,
    xs, part, from_core, from_y, from_x, last_x, last_y, from_z, gate_w, up_w, down_w,
    load_sem, z_send, z_recv, g_send, g_recv, r_send, r_recv, e_send, e_recv,
):
    rows, width = hid_ref.shape
    half = width // 2
    wide = xs.shape[-1]
    sp, tp = (lax.axis_index("sp"), lax.axis_index("tp"))
    z, y = (sp // 2, sp % 2)
    x, c = (tp // 2, tp % 2)
    peer_c = {"sp": sp, "tp": x * 2 + 1 - c}
    peer_x = {"sp": sp, "tp": (1 - x) * 2 + c}
    peer_y = {"sp": z * 2 + 1 - y, "tp": tp}

    def peer_z(k):
        return {"sp": ((z + k) % depth) * 2 + y, "tp": tp}

    def copy(src, dst, send, recv, peer):
        return pltpu.make_async_remote_copy(
            src_ref=src, dst_ref=dst, send_sem=send, recv_sem=recv,
            device_id=peer, device_id_type=pl.DeviceIdType.MESH,
        )

    cols_a, cols_b = (pl.ds(0, half), pl.ds(half, wide - half))
    sum_a, sum_b = (pl.ds(0, half), pl.ds(half, half))
    every = pl.ds(0, rows)

    def ag(k, n):
        sems = (g_send.at[k, n], g_recv.at[k, n])
        if n == 0:
            return copy(xs.at[k, 0], xs.at[k, DX], *sems, peer_x)
        if n == 1:
            return copy(xs.at[k, 0], xs.at[k, DY], *sems, peer_y)
        if n == 2:
            return copy(
                xs.at[k, DX, every, cols_a], xs.at[k, DX + DY, every, cols_a], *sems, peer_y
            )
        if n == 3:
            return copy(
                xs.at[k, DY, every, cols_b], xs.at[k, DX + DY, every, cols_b], *sems, peer_x
            )
        return copy(xs.at[k, n - 4], xs.at[k, DC + n - 4], *sems, peer_c)

    def zg(k):
        return copy(xs.at[0, 0], xs.at[k, 0], z_send.at[k], z_recv.at[k], peer_z(k))

    def rs(k, n):
        sems = (r_send.at[k, n], r_recv.at[k, n])
        if n == 0:
            return copy(part.at[k, pl.ds(DC, DC)], from_core.at[k], *sems, peer_c)
        if n == 1:
            return copy(part.at[k, DY, every, sum_a], from_y.at[k, 0], *sems, peer_y)
        if n == 2:
            return copy(part.at[k, DX + DY, every, sum_a], from_y.at[k, 1], *sems, peer_y)
        if n == 3:
            return copy(part.at[k, DX, every, sum_b], from_x.at[k, 0], *sems, peer_x)
        if n == 4:
            return copy(part.at[k, DX + DY, every, sum_b], from_x.at[k, 1], *sems, peer_x)
        if n == 5:
            return copy(part.at[k, DX, every, sum_a], last_x.at[k], *sems, peer_x)
        return copy(part.at[k, DY, every, sum_b], last_y.at[k], *sems, peer_y)

    def zr(k):
        return copy(part.at[k, 0], from_z.at[k], e_send.at[k], e_recv.at[k], peer_z(depth - k))

    def added(slot, columns, arrived):
        k, s = slot
        now = part[k, s, :, columns].astype(jnp.float32) + arrived.astype(jnp.float32)
        part[k, s, :, columns] = now.astype(jnp.bfloat16)

    loads = [
        pltpu.make_async_copy(gate_hbm.at[0], gate_w, load_sem.at[0]),
        pltpu.make_async_copy(up_hbm.at[0], up_w, load_sem.at[1]),
        pltpu.make_async_copy(down_hbm.at[0], down_w, load_sem.at[2]),
    ]
    own = pltpu.make_async_copy(ext_ref, xs.at[0, 0], load_sem.at[3])
    own.start()
    barrier = pltpu.get_barrier_semaphore()
    peers = [peer_c, peer_x, peer_y] + [peer_z(k) for k in range(1, depth)]
    for peer in peers:
        pl.semaphore_signal(barrier, inc=1, device_id=peer, device_id_type=pl.DeviceIdType.MESH)
    pl.semaphore_wait(barrier, len(peers))
    own.wait()
    for n in (0, 1, 4):
        ag(0, n).start()
    for k in range(1, depth):
        zg(k).start()
    for load in loads:
        load.start()

    block = 4
    lane = lax.broadcasted_iota(jnp.int32, (block * rows, LANES), 1)
    chosen = (lane == sp) | (lane == sp + LANES // 2)

    def compute(k):
        def chunk(j, none):
            held = xs[k, pl.ds(j * block, block)].reshape(block * rows, wide)
            rows_in = held[:, :width]
            weight = jnp.sum(
                jnp.where(chosen, held[:, width:].astype(jnp.float32), 0.0), axis=1, keepdims=True
            )
            g = jnp.dot(rows_in, gate_w[...], preferred_element_type=jnp.float32)
            u = jnp.dot(rows_in, up_w[...], preferred_element_type=jnp.float32)
            act = (clamp_units(g, u) * weight).astype(jnp.bfloat16)
            down = jnp.dot(act, down_w[...], preferred_element_type=jnp.float32)
            part[k, pl.ds(j * block, block)] = down.astype(jnp.bfloat16).reshape(
                block, rows, width
            )
            return none

        lax.fori_loop(0, 2, chunk, 0)

    def step(k, none):
        live, late = (k < depth, k > 0)

        @pl.when(live)
        def _():
            ag(k, 0).wait_recv()
            ag(k, 1).wait_recv()
            for n in (2, 3, 4 + DX, 4 + DY):
                ag(k, n).start()

        @pl.when(k + 1 < depth)
        def _():
            zg(k + 1).wait_recv()
            for n in (0, 1, 4):
                ag(k + 1, n).start()

        @pl.when(late)
        def _():
            p = k - 1
            rs(p, 0).wait_recv()
            for s in range(DC):
                added((p, s), slice(0, width), from_core[p, s])
            for n in (1, 2, 3, 4):
                rs(p, n).start()

        @pl.when(live)
        def _():
            ag(k, 2).wait_recv()
            ag(k, 3).wait_recv()
            ag(k, 4 + DX + DY).start()

        @pl.when(late)
        def _():
            p = k - 1
            for n in (1, 2, 3, 4):
                rs(p, n).wait_recv()
            added((p, DX), slice(0, half), from_y[p, 1])
            added((p, DY), slice(half, width), from_x[p, 1])
            rs(p, 5).start()
            rs(p, 6).start()
            added((p, 0), slice(0, half), from_y[p, 0])
            added((p, 0), slice(half, width), from_x[p, 0])

        @pl.when(k == 0)
        def _():
            for load in loads:
                load.wait()

        @pl.when(live)
        def _():
            for n in (4, 5, 6, 7):
                ag(k, n).wait_recv()
            compute(k)
            rs(k, 0).start()

        @pl.when(late)
        def _():
            p = k - 1
            rs(p, 5).wait_recv()
            rs(p, 6).wait_recv()
            added((p, 0), slice(0, half), last_x[p])
            added((p, 0), slice(half, width), last_y[p])

        @pl.when(k > 1)
        def _():
            zr(k - 1).start()

        return none

    lax.fori_loop(0, depth + 1, step, 0)
    total = hid_ref[...].astype(jnp.float32) + part[0, 0].astype(jnp.float32)
    for k in range(1, depth):
        zr(k).wait_recv()
        total = total + from_z[k].astype(jnp.float32)
    out_ref[...] = total.astype(out_ref.dtype)

    def drain(k, none):
        for n in range(8):
            ag(k, n).wait_send()
        for n in range(7):
            rs(k, n).wait_send()
        return none

    lax.fori_loop(0, depth, drain, 0)
    for k in range(1, depth):
        zg(k).wait_send()
        zr(k).wait_send()


def experts(ext, hidden, expert_gate, expert_up, expert_down):
    depth = lax.axis_size("sp") // 2
    rows, width = hidden.shape
    wide = ext.shape[1]
    kind = jnp.bfloat16
    vmem = pl.BlockSpec(memory_space=pltpu.VMEM)
    hbm = pl.BlockSpec(memory_space=pl.ANY)
    half = width // 2
    dma = pltpu.SemaphoreType.DMA
    return pl.pallas_call(
        functools.partial(moe_kernel, depth),
        out_shape=jax.ShapeDtypeStruct(hidden.shape, kind),
        in_specs=[vmem, vmem, hbm, hbm, hbm],
        out_specs=vmem,
        scratch_shapes=[
            pltpu.VMEM((depth, 8, rows, wide), kind),
            pltpu.VMEM((depth, 8, rows, width), kind),
            pltpu.VMEM((depth, 4, rows, width), kind),
            pltpu.VMEM((depth, 2, rows, half), kind),
            pltpu.VMEM((depth, 2, rows, half), kind),
            pltpu.VMEM((depth, rows, half), kind),
            pltpu.VMEM((depth, rows, half), kind),
            pltpu.VMEM((depth, rows, width), kind),
            pltpu.VMEM(expert_gate.shape[1:], kind),
            pltpu.VMEM(expert_up.shape[1:], kind),
            pltpu.VMEM(expert_down.shape[1:], kind),
            dma((4,)),
            dma((depth,)),
            dma((depth,)),
            dma((depth, 8)),
            dma((depth, 8)),
            dma((depth, 7)),
            dma((depth, 7)),
            dma((depth,)),
            dma((depth,)),
        ],
        compiler_params=pltpu.CompilerParams(
            collective_id=1, has_side_effects=True, vmem_limit_bytes=56 * 1024 * 1024
        ),
    )(ext, hidden, expert_gate, expert_up, expert_down)


def shards(
    conv_input,
    gate_branch,
    conv_taps,
    narrow_maps,
    wide_maps,
    decay_param,
    decay_shift,
    mixer_out,
    stream,
    norm_gain,
    routes,
    route_weights,
    expert_gate,
    expert_up,
    expert_down,
):
    seq_rows, channels = conv_input.shape
    tap_count = conv_taps.shape[0]
    earlier = shifted(conv_input[seq_rows - tap_count + 1 :], "sp", 1)
    head = jnp.zeros((SUBLANES, channels), jnp.float32)
    head = head.at[SUBLANES - tap_count + 1 :].set(earlier.astype(jnp.float32))
    soft = jax.nn.softplus(-decay_param)[None, :]
    factors, local_state = mix_local(
        head, conv_input, conv_taps, narrow_maps, wide_maps, soft, decay_shift
    )
    ends = lax.all_gather(jnp.stack([factors[-1], local_state[-1]]), "sp")
    mine = lax.axis_index("sp")
    state = jnp.zeros((channels,), jnp.float32)
    for position in range(lax.axis_size("sp") - 1):
        longer = ends[position, 0] * state + ends[position, 1]
        state = jnp.where(position < mine, longer, state)
    carried = (None, state)
    recurrent = local_state + factors * carried[1]
    gated_rows = (recurrent * jax.nn.gelu(gate_branch.astype(jnp.float32))).astype(jnp.bfloat16)
    tp_count = lax.axis_size("tp")
    tok_local = seq_rows // tp_count
    mixer_sum = lax.psum_scatter(
        jnp.dot(gated_rows, mixer_out, preferred_element_type=jnp.float32).astype(jnp.bfloat16),
        "tp",
        scatter_dimension=0,
        tiled=True,
    ).astype(jnp.float32)
    hidden_f = stream.astype(jnp.float32) + mixer_sum
    hidden = hidden_f.astype(jnp.bfloat16)
    hidden_f = hidden.astype(jnp.float32)
    normed = (
        hidden_f
        * lax.rsqrt(jnp.mean(hidden_f * hidden_f, axis=-1, keepdims=True) + NORM_EPSILON)
        * norm_gain
    ).astype(jnp.bfloat16)
    model_width = normed.shape[1]
    top_count = routes.shape[1]
    expert_total = expert_gate.shape[0] * lax.axis_size("sp")
    capacity = max(2, 2 * tok_local * top_count // expert_total)
    own_index = lax.axis_index("tp")
    assignments = tok_local * top_count
    own_rows = lax.dynamic_slice_in_dim(routes, own_index * tok_local, tok_local, 0)
    own_weights = lax.dynamic_slice_in_dim(route_weights, own_index * tok_local, tok_local, 0)
    whole_rows = capacity >= tok_local and expert_gate.shape[0] == 1
    if whole_rows and tp_count == 4 and lax.axis_size("sp") % 2 == 0:
        spread = jnp.sum(
            jnp.where(
                own_rows[:, :, None] == jnp.arange(LANES // 2, dtype=jnp.int32)[None, None, :],
                own_weights[:, :, None],
                0.0,
            ),
            axis=1,
        )
        high = lax.reduce_precision(spread, exponent_bits=8, mantissa_bits=7)
        ext = jnp.concatenate(
            [normed, high.astype(jnp.bfloat16), (spread - high).astype(jnp.bfloat16)], axis=1
        )
        return experts(ext, hidden, expert_gate, expert_up, expert_down)
    own_routes = own_rows.reshape(assignments)
    own_ranks = slot_ranks(own_routes[None, :], expert_total)[0]
    source = jnp.arange(assignments, dtype=jnp.int32) // top_count
    slot_source = (
        jnp.full((expert_total * capacity,), -1, jnp.int32)
        .at[own_routes * capacity + own_ranks]
        .set(source)
    )
    outgoing = take_rows(normed, slot_source).reshape(expert_total, 1, capacity, model_width)
    partial_value = expert_work(
        lax.all_gather(
            lax.all_to_all(outgoing, "sp", split_axis=0, concat_axis=0, tiled=True),
            "tp",
            axis=1,
            tiled=True,
        ),
        expert_gate,
        expert_up,
        expert_down,
    )
    summed = lax.psum_scatter(
        partial_value.astype(jnp.bfloat16), "tp", scatter_dimension=1, tiled=True
    )
    returned = lax.all_to_all(summed, "sp", split_axis=0, concat_axis=0, tiled=True)
    own_slots = own_routes * capacity + own_ranks
    picked = returned.reshape(expert_total * capacity, model_width)[own_slots]
    own_weights = lax.dynamic_slice_in_dim(route_weights, own_index * tok_local, tok_local, 0)
    combined = jnp.sum(
        picked.reshape(tok_local, top_count, model_width).astype(jnp.float32)
        * own_weights[:, :, None],
        axis=1,
    )
    return (hidden_f + combined).astype(jnp.bfloat16)


def solution(mesh):
    placed = (
        P("sp", "tp"),
        P("sp", "tp"),
        P(None, "tp"),
        P(None, "tp", None, None),
        P(None, "tp", None, None),
        P("tp"),
        P("sp", "tp"),
        P("tp", None),
        P(("sp", "tp"), None),
        P(),
        P("sp", None),
        P("sp", None),
        P("sp", None, "tp"),
        P("sp", None, "tp"),
        P("sp", "tp", None),
    )
    return jax.shard_map(
        shards, mesh=mesh, in_specs=placed, out_specs=P(("sp", "tp"), None), check_vma=False
    )
```

```python
import functools

import jax
import jax.numpy as jnp
from jax import lax
from jax.experimental import pallas as pl
from jax.experimental.pallas import tpu as pltpu
from jax.sharding import PartitionSpec as P

NORM_EPSILON = 1e-06
CLAMP_LIMIT = 7.0
GATE_SLOPE = 1.702
DECAY_SCALE = 8.0


def shifted(block, axis, distance):
    devices = range(lax.axis_size(axis))
    route = [(i - distance, i) for i in devices if i - distance in devices]
    return lax.ppermute(block, axis, route)


def clamp_units(gate_pre, up_pre):
    clamped = jnp.minimum(gate_pre, CLAMP_LIMIT)
    upper = jnp.clip(up_pre, -CLAMP_LIMIT, CLAMP_LIMIT)
    return (upper + 1.0) * clamped * jax.nn.sigmoid(GATE_SLOPE * clamped)


def slot_ranks(flat_routes, expert_total):
    onehot = (
        flat_routes[:, :, None] == jnp.arange(expert_total, dtype=jnp.int32)[None, None, :]
    ).astype(jnp.int32)
    return jnp.sum(jnp.cumsum(onehot, axis=1) * onehot, axis=2) - 1


def take_rows(source_rows, slot_source):
    filled = slot_source >= 0
    picked = source_rows[jnp.maximum(slot_source, 0)]
    return jnp.where(filled[:, None], picked, jnp.zeros_like(picked))


def expert_work(arrived, expert_gate, expert_up, expert_down):
    local_experts = expert_gate.shape[0]
    buffer_shape = arrived.shape
    grouped = arrived.reshape(
        buffer_shape[0] // local_experts,
        local_experts,
        buffer_shape[1] * buffer_shape[2],
        buffer_shape[3],
    )
    gate_pre = jnp.einsum(
        "sxcd,xdf->sxcf", grouped, expert_gate, preferred_element_type=jnp.float32
    )
    up_pre = jnp.einsum("sxcd,xdf->sxcf", grouped, expert_up, preferred_element_type=jnp.float32)
    activation = clamp_units(gate_pre, up_pre).astype(jnp.bfloat16)
    partial_value = jnp.einsum(
        "sxcf,xfd->sxcd", activation, expert_down, preferred_element_type=jnp.float32
    )
    return partial_value.reshape(buffer_shape)


LANES = 128
SUBLANES = 8
DX, DY, DC = 1, 2, 4
SERIES_LIMIT = 0.05
GELU_SCALE = 0.7978845608028654
GELU_CUBIC = 0.044715


def mix_kernel(
    head_ref, conv_ref, taps_ref, narrow_ref, wide_ref, soft_ref, shift_ref,
    factor_ref, state_ref, padded, log_keep, drive_keep,
):
    rows, channels = conv_ref.shape
    taps = taps_ref.shape[0]
    padded[0:SUBLANES, :] = head_ref[...]
    padded[SUBLANES:, :] = conv_ref[...].astype(jnp.float32)
    total = jnp.zeros((rows, channels), jnp.float32)
    for k in range(taps):
        total = total + padded[pl.ds(SUBLANES - taps + 1 + k, rows), :] * taps_ref[k : k + 1, :]
    convolved = total.astype(jnp.bfloat16)
    narrow_size, wide_size = narrow_ref.shape[2], wide_ref.shape[2]
    spans = []
    for j in range(wide_ref.shape[1]):
        base = j * (2 * narrow_size + wide_size)
        spans.append((base, narrow_size, narrow_ref, 2 * j))
        spans.append((base + narrow_size, narrow_size, narrow_ref, 2 * j + 1))
        spans.append((base + 2 * narrow_size, wide_size, wide_ref, j))
    for start, size, maps, head in spans:
        piece = convolved[:, start : start + size]
        decay_pre = jnp.dot(piece, maps[0, head], preferred_element_type=jnp.float32)
        input_pre = jnp.dot(piece, maps[1, head], preferred_element_type=jnp.float32)
        cols = slice(start, start + size)
        log_decay = (
            -DECAY_SCALE * jax.nn.sigmoid(decay_pre) * soft_ref[:, cols] + shift_ref[:, cols]
        )
        decay = jnp.exp(log_decay)
        y = 2.0 * log_decay
        series = -y * (1.0 + y * (0.5 + y * (1.0 / 6.0 + y * (1.0 / 24.0 + y * (1.0 / 120.0)))))
        lost = jnp.where(y > -SERIES_LIMIT, series, 1.0 - decay * decay)
        log_keep[:, cols] = decay
        drive_keep[:, cols] = (
            jnp.sqrt(lost) * jax.nn.sigmoid(input_pre) * piece.astype(jnp.float32)
        )
    row_id = lax.broadcasted_iota(jnp.int32, (SUBLANES, channels), 0)

    def tile(i, carry):
        product, state = carry
        at = pl.ds(pl.multiple_of(i * SUBLANES, SUBLANES), SUBLANES)
        a, b = log_keep[at, :], drive_keep[at, :]
        step = 1
        while step < SUBLANES:
            inside = row_id >= step
            a_before = jnp.where(inside, pltpu.roll(a, step, 0), 1.0)
            b_before = jnp.where(inside, pltpu.roll(b, step, 0), 0.0)
            b = a * b_before + b
            a = a * a_before
            step *= 2
        b = b + a * state
        a = a * product
        factor_ref[at, :] = a
        state_ref[at, :] = b
        last = slice(SUBLANES - 1, SUBLANES)
        return (a[last, :], b[last, :])

    lax.fori_loop(
        0,
        rows // SUBLANES,
        tile,
        (jnp.ones((1, channels), jnp.float32), jnp.zeros((1, channels), jnp.float32)),
    )


def mix_local(head, conv_input, conv_taps, narrow_maps, wide_maps, soft, decay_shift):
    shape = conv_input.shape
    flat = jax.ShapeDtypeStruct(shape, jnp.float32)
    return pl.pallas_call(
        mix_kernel,
        out_shape=(flat, flat),
        in_specs=[pl.BlockSpec(memory_space=pltpu.VMEM)] * 7,
        out_specs=(pl.BlockSpec(memory_space=pltpu.VMEM),) * 2,
        scratch_shapes=[
            pltpu.VMEM((shape[0] + SUBLANES, shape[1]), jnp.float32),
            pltpu.VMEM(shape, jnp.float32),
            pltpu.VMEM(shape, jnp.float32),
        ],
        compiler_params=pltpu.CompilerParams(vmem_limit_bytes=32 * 1024 * 1024),
    )(head, conv_input, conv_taps, narrow_maps, wide_maps, soft, decay_shift)


def front_kernel(
    count, conv_ref, gate_ref, taps_ref, narrow_ref, wide_ref, soft_ref, shift_ref, mixer_hbm,
    stream_ref, gain_ref, spread_ref, hid_ref, ext_ref,
    head, factor, state, padded, log_keep, drive_keep, halo, ends, gated, mixer, mix, arrived,
    load_sem, halo_send, halo_recv, end_send, end_recv, mix_send, mix_recv,
):
    rows = conv_ref.shape[0]
    kept, width = stream_ref.shape
    sp, tp = (lax.axis_index("sp"), lax.axis_index("tp"))
    x, c = (tp // 2, tp % 2)
    mesh_id = pl.DeviceIdType.MESH

    def later(k):
        return {"sp": (sp + k) % count, "tp": tp}

    over_x = {"sp": sp, "tp": (1 - x) * 2 + c}
    over_both = {"sp": sp, "tp": (1 - x) * 2 + 1 - c}
    over_c = {"sp": sp, "tp": x * 2 + 1 - c}
    load = pltpu.make_async_copy(mixer_hbm, mixer, load_sem)
    load.start()
    barrier = pltpu.get_barrier_semaphore()
    peers = [over_x, over_both, over_c] + [later(k) for k in range(1, count)]
    for peer in peers:
        pl.semaphore_signal(barrier, inc=1, device_id=peer, device_id_type=mesh_id)
    pl.semaphore_wait(barrier, len(peers))
    halo_rows = halo.shape[0]
    halo_copy = pltpu.make_async_remote_copy(
        src_ref=conv_ref.at[pl.ds(rows - halo_rows, halo_rows)], dst_ref=halo,
        send_sem=halo_send, recv_sem=halo_recv, device_id=later(1), device_id_type=mesh_id,
    )
    halo_copy.start()
    halo_copy.wait()
    before = halo[...].astype(jnp.float32)[halo_rows - SUBLANES :]
    head[...] = jnp.where(sp > 0, before, jnp.zeros_like(before))
    mix_kernel(
        head, conv_ref, taps_ref, narrow_ref, wide_ref, soft_ref, shift_ref,
        factor, state, padded, log_keep, drive_keep,
    )
    ends[0, 0:SUBLANES, :] = factor[rows - SUBLANES :, :]
    ends[0, SUBLANES:, :] = state[rows - SUBLANES :, :]
    end_copies = [
        pltpu.make_async_remote_copy(
            src_ref=ends.at[0], dst_ref=ends.at[k], send_sem=end_send.at[k],
            recv_sem=end_recv.at[k], device_id=later(k), device_id_type=mesh_id,
        )
        for k in range(1, count)
    ]
    for one in end_copies:
        one.start()
    g = gate_ref[...].astype(jnp.float32)
    log_keep[...] = 0.5 * g * (1.0 + jnp.tanh(GELU_SCALE * (g + GELU_CUBIC * g * g * g)))
    load.wait()
    for one in end_copies:
        one.wait()
    last_factor, last_state = (SUBLANES - 1, 2 * SUBLANES - 1)
    carry = jnp.zeros((1, conv_ref.shape[1]), jnp.float32)
    for k in range(count - 1, 0, -1):
        longer = (
            ends[k, last_factor : last_factor + 1, :] * carry
            + ends[k, last_state : last_state + 1, :]
        )
        carry = jnp.where(sp >= k, longer, carry)
    recurrent = state[...] + factor[...] * carry
    gated[...] = (recurrent * log_keep[...]).astype(jnp.bfloat16)

    def project(chip, slot):
        some = gated[pl.ds(pl.multiple_of(chip * 2 * kept, 2 * kept), 2 * kept), :]
        value = jnp.dot(some, mixer[...], preferred_element_type=jnp.float32)
        mix[slot : slot + 2] = value.astype(jnp.bfloat16).reshape(2, kept, width)

    def give(n, source, peer):
        return pltpu.make_async_remote_copy(
            src_ref=mix.at[source], dst_ref=arrived.at[n], send_sem=mix_send.at[n],
            recv_sem=mix_recv.at[n], device_id=peer, device_id_type=mesh_id,
        )

    given = [give(0, c, over_x), give(1, 1 - c, over_both), give(2, 3 - c, over_c)]
    project(1 - x, 0)
    given[0].start()
    given[1].start()
    project(x, 2)
    given[2].start()
    total = mix[2 + c].astype(jnp.float32)
    for n in (2, 0, 1):
        given[n].wait()
        total = total + arrived[n].astype(jnp.float32)
    hidden = (stream_ref[...].astype(jnp.float32) + total).astype(jnp.bfloat16)
    hid_ref[...] = hidden
    wide = hidden.astype(jnp.float32)
    mean = jnp.mean(wide * wide, axis=-1, keepdims=True)
    normed = wide * lax.rsqrt(mean + NORM_EPSILON) * gain_ref[...]
    ext_ref[:, :width] = normed.astype(jnp.bfloat16)
    ext_ref[:, width:] = spread_ref[...]


def front(
    conv_input, gate_branch, conv_taps, narrow_maps, wide_maps, soft, decay_shift, mixer_out,
    stream, norm_gain, spread,
):
    count = lax.axis_size("sp")
    rows, channels = conv_input.shape
    kept, width = stream.shape
    single, kind = (jnp.float32, jnp.bfloat16)
    vmem = pl.BlockSpec(memory_space=pltpu.VMEM)
    dma = pltpu.SemaphoreType.DMA
    return pl.pallas_call(
        functools.partial(front_kernel, count),
        out_shape=(
            jax.ShapeDtypeStruct((kept, width), kind),
            jax.ShapeDtypeStruct((kept, width + LANES), kind),
        ),
        in_specs=[vmem] * 7 + [pl.BlockSpec(memory_space=pl.ANY)] + [vmem] * 3,
        out_specs=(vmem, vmem),
        scratch_shapes=[
            pltpu.VMEM((SUBLANES, channels), single),
            pltpu.VMEM((rows, channels), single),
            pltpu.VMEM((rows, channels), single),
            pltpu.VMEM((rows + SUBLANES, channels), single),
            pltpu.VMEM((rows, channels), single),
            pltpu.VMEM((rows, channels), single),
            pltpu.VMEM((2 * SUBLANES, channels), kind),
            pltpu.VMEM((count, 2 * SUBLANES, channels), single),
            pltpu.VMEM((rows, channels), kind),
            pltpu.VMEM(mixer_out.shape, kind),
            pltpu.VMEM((4, kept, width), kind),
            pltpu.VMEM((3, kept, width), kind),
            dma,
            dma,
            dma,
            dma((count,)),
            dma((count,)),
            dma((3,)),
            dma((3,)),
        ],
        compiler_params=pltpu.CompilerParams(
            collective_id=2, has_side_effects=True, vmem_limit_bytes=40 * 1024 * 1024
        ),
    )(
        conv_input, gate_branch, conv_taps, narrow_maps, wide_maps, soft, decay_shift, mixer_out,
        stream, norm_gain, spread,
    )


def moe_kernel(
    depth, ext_ref, hid_ref, gate_hbm, up_hbm, down_hbm, out_ref,
    xs, part, from_core, from_y, from_x, last_x, last_y, from_z, gate_w, up_w, down_w,
    load_sem, z_send, z_recv, g_send, g_recv, r_send, r_recv, e_send, e_recv,
):
    rows, width = hid_ref.shape
    half = width // 2
    wide = xs.shape[-1]
    sp, tp = (lax.axis_index("sp"), lax.axis_index("tp"))
    z, y = (sp // 2, sp % 2)
    x, c = (tp // 2, tp % 2)
    peer_c = {"sp": sp, "tp": x * 2 + 1 - c}
    peer_x = {"sp": sp, "tp": (1 - x) * 2 + c}
    peer_y = {"sp": z * 2 + 1 - y, "tp": tp}

    def peer_z(k):
        return {"sp": ((z + k) % depth) * 2 + y, "tp": tp}

    def copy(src, dst, send, recv, peer):
        return pltpu.make_async_remote_copy(
            src_ref=src, dst_ref=dst, send_sem=send, recv_sem=recv,
            device_id=peer, device_id_type=pl.DeviceIdType.MESH,
        )

    cols_a, cols_b = (pl.ds(0, half), pl.ds(half, wide - half))
    sum_a, sum_b = (pl.ds(0, half), pl.ds(half, half))
    every = pl.ds(0, rows)

    def ag(k, n):
        sems = (g_send.at[k, n], g_recv.at[k, n])
        if n == 0:
            return copy(xs.at[k, 0], xs.at[k, DX], *sems, peer_x)
        if n == 1:
            return copy(xs.at[k, 0], xs.at[k, DY], *sems, peer_y)
        if n == 2:
            return copy(
                xs.at[k, DX, every, cols_a], xs.at[k, DX + DY, every, cols_a], *sems, peer_y
            )
        if n == 3:
            return copy(
                xs.at[k, DY, every, cols_b], xs.at[k, DX + DY, every, cols_b], *sems, peer_x
            )
        return copy(xs.at[k, n - 4], xs.at[k, DC + n - 4], *sems, peer_c)

    def zg(k):
        return copy(xs.at[0, 0], xs.at[k, 0], z_send.at[k], z_recv.at[k], peer_z(k))

    def rs(k, n):
        sems = (r_send.at[k, n], r_recv.at[k, n])
        if n == 0:
            return copy(part.at[k, pl.ds(DC, DC)], from_core.at[k], *sems, peer_c)
        if n == 1:
            return copy(part.at[k, DY, every, sum_a], from_y.at[k, 0], *sems, peer_y)
        if n == 2:
            return copy(part.at[k, DX + DY, every, sum_a], from_y.at[k, 1], *sems, peer_y)
        if n == 3:
            return copy(part.at[k, DX, every, sum_b], from_x.at[k, 0], *sems, peer_x)
        if n == 4:
            return copy(part.at[k, DX + DY, every, sum_b], from_x.at[k, 1], *sems, peer_x)
        if n == 5:
            return copy(part.at[k, DX, every, sum_a], last_x.at[k], *sems, peer_x)
        return copy(part.at[k, DY, every, sum_b], last_y.at[k], *sems, peer_y)

    def zr(k):
        return copy(part.at[k, 0], from_z.at[k], e_send.at[k], e_recv.at[k], peer_z(depth - k))

    def added(slot, columns, arrived):
        k, s = slot
        now = part[k, s, :, columns].astype(jnp.float32) + arrived.astype(jnp.float32)
        part[k, s, :, columns] = now.astype(jnp.bfloat16)

    loads = [
        pltpu.make_async_copy(gate_hbm.at[0], gate_w, load_sem.at[0]),
        pltpu.make_async_copy(up_hbm.at[0], up_w, load_sem.at[1]),
        pltpu.make_async_copy(down_hbm.at[0], down_w, load_sem.at[2]),
    ]
    own = pltpu.make_async_copy(ext_ref, xs.at[0, 0], load_sem.at[3])
    own.start()
    barrier = pltpu.get_barrier_semaphore()
    peers = [peer_c, peer_x, peer_y] + [peer_z(k) for k in range(1, depth)]
    for peer in peers:
        pl.semaphore_signal(barrier, inc=1, device_id=peer, device_id_type=pl.DeviceIdType.MESH)
    pl.semaphore_wait(barrier, len(peers))
    own.wait()
    for n in (0, 1, 4):
        ag(0, n).start()
    for k in range(1, depth):
        zg(k).start()
    for load in loads:
        load.start()

    block = 4
    lane = lax.broadcasted_iota(jnp.int32, (block * rows, LANES), 1)
    chosen = (lane == sp) | (lane == sp + LANES // 2)

    def compute(k):
        def chunk(i, none):
            j = 1 - i
            held = xs[k, pl.ds(j * block, block)].reshape(block * rows, wide)
            rows_in = held[:, :width]
            weight = jnp.sum(
                jnp.where(chosen, held[:, width:].astype(jnp.float32), 0.0), axis=1, keepdims=True
            )
            g = jnp.dot(rows_in, gate_w[...], preferred_element_type=jnp.float32)
            u = jnp.dot(rows_in, up_w[...], preferred_element_type=jnp.float32)
            act = (clamp_units(g, u) * weight).astype(jnp.bfloat16)
            down = jnp.dot(act, down_w[...], preferred_element_type=jnp.float32)
            part[k, pl.ds(j * block, block)] = down.astype(jnp.bfloat16).reshape(
                block, rows, width
            )

            @pl.when(i == 0)
            def _():
                rs(k, 0).start()

            return none

        lax.fori_loop(0, 2, chunk, 0)

    def step(k, none):
        live, late = (k < depth, k > 0)

        @pl.when(live)
        def _():
            ag(k, 0).wait_recv()
            ag(k, 1).wait_recv()
            for n in (2, 3, 4 + DX, 4 + DY):
                ag(k, n).start()

        @pl.when(k + 1 < depth)
        def _():
            zg(k + 1).wait_recv()
            for n in (0, 1, 4):
                ag(k + 1, n).start()

        @pl.when(live)
        def _():
            ag(k, 2).wait_recv()
            ag(k, 3).wait_recv()
            ag(k, 4 + DX + DY).start()

        @pl.when(late)
        def _():
            p = k - 1
            for n in (1, 2, 3, 4):
                rs(p, n).wait_recv()
            added((p, DX), slice(0, half), from_y[p, 1])
            added((p, DY), slice(half, width), from_x[p, 1])
            rs(p, 5).start()
            rs(p, 6).start()
            added((p, 0), slice(0, half), from_y[p, 0])
            added((p, 0), slice(half, width), from_x[p, 0])

        @pl.when(k == 0)
        def _():
            for load in loads:
                load.wait()

        @pl.when(live)
        def _():
            for n in (4, 5, 6, 7):
                ag(k, n).wait_recv()
            compute(k)
            rs(k, 0).wait_recv()
            for s in range(DC):
                added((k, s), slice(0, width), from_core[k, s])
            for n in (1, 2, 3, 4):
                rs(k, n).start()

        @pl.when(late)
        def _():
            p = k - 1
            rs(p, 5).wait_recv()
            rs(p, 6).wait_recv()
            added((p, 0), slice(0, half), last_x[p])
            added((p, 0), slice(half, width), last_y[p])

        @pl.when(k > 1)
        def _():
            zr(k - 1).start()

        return none

    lax.fori_loop(0, depth + 1, step, 0)
    total = hid_ref[...].astype(jnp.float32) + part[0, 0].astype(jnp.float32)
    for k in range(1, depth):
        zr(k).wait_recv()
        total = total + from_z[k].astype(jnp.float32)
    out_ref[...] = total.astype(out_ref.dtype)

    def drain(k, none):
        for n in range(8):
            ag(k, n).wait_send()
        for n in range(7):
            rs(k, n).wait_send()
        return none

    lax.fori_loop(0, depth, drain, 0)
    for k in range(1, depth):
        zg(k).wait_send()
        zr(k).wait_send()


def experts(ext, hidden, expert_gate, expert_up, expert_down):
    depth = lax.axis_size("sp") // 2
    rows, width = hidden.shape
    wide = ext.shape[1]
    kind = jnp.bfloat16
    vmem = pl.BlockSpec(memory_space=pltpu.VMEM)
    hbm = pl.BlockSpec(memory_space=pl.ANY)
    half = width // 2
    dma = pltpu.SemaphoreType.DMA
    return pl.pallas_call(
        functools.partial(moe_kernel, depth),
        out_shape=jax.ShapeDtypeStruct(hidden.shape, kind),
        in_specs=[vmem, vmem, hbm, hbm, hbm],
        out_specs=vmem,
        scratch_shapes=[
            pltpu.VMEM((depth, 8, rows, wide), kind),
            pltpu.VMEM((depth, 8, rows, width), kind),
            pltpu.VMEM((depth, 4, rows, width), kind),
            pltpu.VMEM((depth, 2, rows, half), kind),
            pltpu.VMEM((depth, 2, rows, half), kind),
            pltpu.VMEM((depth, rows, half), kind),
            pltpu.VMEM((depth, rows, half), kind),
            pltpu.VMEM((depth, rows, width), kind),
            pltpu.VMEM(expert_gate.shape[1:], kind),
            pltpu.VMEM(expert_up.shape[1:], kind),
            pltpu.VMEM(expert_down.shape[1:], kind),
            dma((4,)),
            dma((depth,)),
            dma((depth,)),
            dma((depth, 8)),
            dma((depth, 8)),
            dma((depth, 7)),
            dma((depth, 7)),
            dma((depth,)),
            dma((depth,)),
        ],
        compiler_params=pltpu.CompilerParams(
            collective_id=1, has_side_effects=True, vmem_limit_bytes=56 * 1024 * 1024
        ),
    )(ext, hidden, expert_gate, expert_up, expert_down)


def shards(
    conv_input,
    gate_branch,
    conv_taps,
    narrow_maps,
    wide_maps,
    decay_param,
    decay_shift,
    mixer_out,
    stream,
    norm_gain,
    routes,
    route_weights,
    expert_gate,
    expert_up,
    expert_down,
):
    seq_rows, channels = conv_input.shape
    tap_count = conv_taps.shape[0]
    tp_count = lax.axis_size("tp")
    tok_local = seq_rows // tp_count
    top_count = routes.shape[1]
    expert_total = expert_gate.shape[0] * lax.axis_size("sp")
    capacity = max(2, 2 * tok_local * top_count // expert_total)
    own_index = lax.axis_index("tp")
    own_rows = lax.dynamic_slice_in_dim(routes, own_index * tok_local, tok_local, 0)
    own_weights = lax.dynamic_slice_in_dim(route_weights, own_index * tok_local, tok_local, 0)
    soft = jax.nn.softplus(-decay_param)[None, :]
    whole_rows = capacity >= tok_local and expert_gate.shape[0] == 1
    if whole_rows and tp_count == 4 and lax.axis_size("sp") % 2 == 0:
        lane = jnp.arange(LANES, dtype=jnp.int32)
        spread = jnp.sum(
            jnp.where(
                own_rows[:, :, None] == (lane % (LANES // 2))[None, None, :],
                own_weights[:, :, None],
                0.0,
            ),
            axis=1,
        )
        high = lax.reduce_precision(spread, exponent_bits=8, mantissa_bits=7)
        pair = jnp.where(lane[None, :] < LANES // 2, high, spread - high).astype(jnp.bfloat16)
        hidden, ext = front(
            conv_input, gate_branch, conv_taps, narrow_maps, wide_maps, soft, decay_shift,
            mixer_out, stream, norm_gain[None, :], pair,
        )
        return experts(ext, hidden, expert_gate, expert_up, expert_down)
    earlier = shifted(conv_input[seq_rows - tap_count + 1 :], "sp", 1)
    head = jnp.zeros((SUBLANES, channels), jnp.float32)
    head = head.at[SUBLANES - tap_count + 1 :].set(earlier.astype(jnp.float32))
    factors, local_state = mix_local(
        head, conv_input, conv_taps, narrow_maps, wide_maps, soft, decay_shift
    )
    ends = lax.all_gather(jnp.stack([factors[-1], local_state[-1]]), "sp")
    mine = lax.axis_index("sp")
    state = jnp.zeros((channels,), jnp.float32)
    for position in range(lax.axis_size("sp") - 1):
        longer = ends[position, 0] * state + ends[position, 1]
        state = jnp.where(position < mine, longer, state)
    carried = (None, state)
    recurrent = local_state + factors * carried[1]
    gated_rows = (recurrent * jax.nn.gelu(gate_branch.astype(jnp.float32))).astype(jnp.bfloat16)
    mixer_sum = lax.psum_scatter(
        jnp.dot(gated_rows, mixer_out, preferred_element_type=jnp.float32).astype(jnp.bfloat16),
        "tp",
        scatter_dimension=0,
        tiled=True,
    ).astype(jnp.float32)
    hidden_f = stream.astype(jnp.float32) + mixer_sum
    hidden = hidden_f.astype(jnp.bfloat16)
    hidden_f = hidden.astype(jnp.float32)
    normed = (
        hidden_f
        * lax.rsqrt(jnp.mean(hidden_f * hidden_f, axis=-1, keepdims=True) + NORM_EPSILON)
        * norm_gain
    ).astype(jnp.bfloat16)
    model_width = normed.shape[1]
    assignments = tok_local * top_count
    own_routes = own_rows.reshape(assignments)
    own_ranks = slot_ranks(own_routes[None, :], expert_total)[0]
    source = jnp.arange(assignments, dtype=jnp.int32) // top_count
    slot_source = (
        jnp.full((expert_total * capacity,), -1, jnp.int32)
        .at[own_routes * capacity + own_ranks]
        .set(source)
    )
    outgoing = take_rows(normed, slot_source).reshape(expert_total, 1, capacity, model_width)
    partial_value = expert_work(
        lax.all_gather(
            lax.all_to_all(outgoing, "sp", split_axis=0, concat_axis=0, tiled=True),
            "tp",
            axis=1,
            tiled=True,
        ),
        expert_gate,
        expert_up,
        expert_down,
    )
    summed = lax.psum_scatter(
        partial_value.astype(jnp.bfloat16), "tp", scatter_dimension=1, tiled=True
    )
    returned = lax.all_to_all(summed, "sp", split_axis=0, concat_axis=0, tiled=True)
    own_slots = own_routes * capacity + own_ranks
    picked = returned.reshape(expert_total * capacity, model_width)[own_slots]
    combined = jnp.sum(
        picked.reshape(tok_local, top_count, model_width).astype(jnp.float32)
        * own_weights[:, :, None],
        axis=1,
    )
    return (hidden_f + combined).astype(jnp.bfloat16)


def solution(mesh):
    placed = (
        P("sp", "tp"),
        P("sp", "tp"),
        P(None, "tp"),
        P(None, "tp", None, None),
        P(None, "tp", None, None),
        P("tp"),
        P("sp", "tp"),
        P("tp", None),
        P(("sp", "tp"), None),
        P(),
        P("sp", None),
        P("sp", None),
        P("sp", None, "tp"),
        P("sp", None, "tp"),
        P("sp", "tp", None),
    )
    return jax.shard_map(
        shards, mesh=mesh, in_specs=placed, out_specs=P(("sp", "tp"), None), check_vma=False
    )
```
